32 devices in a mesh: grp: 2 (over y), ep: 8 (over z, x), tp: 2 (over core).
Axes of the slice: x: 2, y: 2, z: 4, core: 2. Of those that a mesh axis runs over, the one named last changes fastest.
Arguments:
- tokens: bfloat16 [512, 2048], P(('grp', 'ep'), 'tp'), parts along dimension 0, may hold values from -6 to 6
- gain: float32 [2048], replicated, may hold values from 0.1 to 1.9
- routes: int32 [512, 4], P(('grp', 'ep')), parts along dimension 0, may hold values from 0 to 7, all different within a row; in each aligned block of 32 rows (0 to 31, 32 to 63, ...) at most 32 rows name the same one
- weights: float32 [512, 4], P(('grp', 'ep')), parts along dimension 0, may hold values from 0.05 to 1
- w_gate: bfloat16 [8, 2048, 6144], P('ep', None, 'tp'), may hold values from -0.125 to 0.125
- w_up: bfloat16 [8, 2048, 6144], P('ep', None, 'tp'), may hold values from -0.125 to 0.125
- w_down: bfloat16 [8, 6144, 2048], P('ep', 'tp'), may hold values from -0.078125 to 0.078125
Outputs:
- mixed: bfloat16 [512, 2048], P(('grp', 'ep'), 'tp'), parts along dimension 0
The draws below stay inside these ranges and needn't reach their ends.
There are 2 independent parts, one for each index of `grp`. The reference program is written for one: setup_inputs(seed, part) draws one part's arguments, and reference() takes and returns one part's arrays. A program takes and returns all parts, laid end to end along the dimension named above; an argument that names none is the same for every part. Nothing has to cross between parts.
Inputs may be any that keep to these rules, and one draw needn't show every extreme that they name: `routes`: each row names 4 different experts. Among the rows of one device no expert is named by more than 32 rows, a bound that some block reaches.
All inputs are finite; a program needn't handle non-finite values.
Results may differ from the reference program's by a relative error of at most 0.019.
Values may be sent and summed in bfloat16 or wider, within the bound.
A program may use at most 128 MiB of HBM per device.

```python
import math
import jax
import jax.numpy as jnp
import numpy as np
from jax import lax

D = 2048
FF = 6144
TOP = 4
TOK_DEV = 32
EXPERTS = 8
CAP = 32
TOKENS = 256
N_EP = 8
N_TP = 2


def levels(own_key, shape, pieces, smallest, high):
    level = 1.0
    for axis_at, blocks in pieces:
        steps = jax.random.uniform(jax.random.fold_in(jax.random.fold_in(own_key, 6), axis_at), (blocks,), jnp.float32, smallest / len(pieces), high / len(pieces))
        level = level * jnp.repeat(jnp.exp(steps), shape[axis_at] // blocks).reshape((-1,) + (1,) * (len(shape) - 1 - axis_at))
    return level


def routed_block(rng, own, number, rows, number_of, top, most, skew):
    sequence = jax.random.permutation(rng, number_of)
    heavy_load, ordinary = portions_of(number_of, rows * top, most, skew, True), portions_of(number_of, rows * top, most, skew, False)
    places = jnp.arange(number_of)

    def named(tallies, offset_by):
        used = int((tallies > 0).sum())
        fixed = max(1, used // 4)
        moved = fixed + (places - fixed + offset_by * (used - fixed)) % max(1, number_of - fixed)
        return jnp.zeros((number_of,), jnp.int32).at[sequence[jnp.where(places < fixed, places, moved)]].set(jnp.asarray(tallies, jnp.int32))

    tallies = jnp.where(number % 4 == 0, named(heavy_load, number // 4), named(ordinary, number - number // 4 - 1))
    mixed = jax.random.permutation(jax.random.fold_in(own, 3), number_of)
    giver, receiver = mixed[0:number_of // 2 * 2:2], mixed[1:number_of // 2 * 2:2]
    slack = jnp.minimum(tallies[giver] - 1, most - tallies[receiver]) // 2
    slack = jnp.where((giver == sequence[0]) | (receiver == sequence[0]) | (tallies[receiver] == 0), 0, jnp.maximum(slack, 0))
    moved = jax.random.randint(jax.random.fold_in(own, 4), (number_of // 2,), 0, 1 << 20) % (slack + 1)
    tallies = tallies.at[giver].add(-moved).at[receiver].add(moved)
    items = jnp.searchsorted(jnp.cumsum(tallies), jnp.arange(rows * top), side="right").astype(jnp.int32)
    listing = items.reshape(top, rows).T
    listing = listing[jax.random.permutation(jax.random.fold_in(own, 1), rows)]
    offset_by = jax.random.randint(jax.random.fold_in(own, 2), (rows, 1), 0, top)
    return jnp.take_along_axis(listing, (jnp.arange(top)[None, :] + offset_by) % top, axis=1)


def portions_of(count, total, most, lean, full):
    weights = [(1 << 20) // math.isqrt(grade ** lean) + 1 for grade in range(1, count + 1)]
    largest = most if full else min(most, max(-(-total // count), total * weights[0] // sum(weights)))
    least = 1 if total - largest >= count - 1 else 0
    given, surplus = [largest] + [least] * (count - 1), total - largest - least * (count - 1)
    while surplus > 0:
        free = [i for i in range(1, count) if given[i] < largest] or [i for i in range(1, count) if given[i] < most]
        whole, budget = sum([weights[i] for i in free]), surplus
        for i in free:
            extra = min(most - given[i], max(1, budget * weights[i] // whole), surplus)
            given[i] = given[i] + extra
            surplus = surplus - extra
    return np.array(given)


def noise(rng, shape, scale, limit, split=(), held_as=jnp.bfloat16):
    result = scale * jax.random.normal(rng, shape, jnp.float32)
    if split:
        result = result * levels(rng, shape, split, -0.22, 0.18)
    return jnp.clip(result, -limit, limit).astype(held_as)


def setup_inputs(seed: int = 0, part: int = 0) -> dict:
    seeds = jax.random.split(jax.random.key(seed), 8)
    own_keys = jax.random.split(jax.random.fold_in(seeds[7], part), 8)
    tokens = noise(own_keys[0], (TOKENS, D), 1.0, 6.0, ((0, 8), (1, 2)))
    gain = jnp.clip(1.0 + 0.18 * jax.random.normal(seeds[1], (D,), jnp.float32), 0.1, 1.9)
    routes_keys = jax.random.split(jax.random.fold_in(own_keys[2], 1), TOKENS // TOK_DEV)
    routes_turns = jax.random.permutation(jax.random.fold_in(own_keys[2], 3), TOKENS // TOK_DEV)
    routes = jax.vmap(lambda own, number: routed_block(jax.random.fold_in(own_keys[2], 2), own, number, TOK_DEV, EXPERTS, TOP, CAP, 2))(routes_keys, routes_turns).reshape((TOKENS, TOP))
    weights = jnp.clip(jnp.exp(math.log(1.0) - 2.9957323 * jax.random.uniform(own_keys[3], (TOKENS, TOP), jnp.float32) ** levels(own_keys[3], (TOKENS, TOP), ((0, 8),), -0.2, 0.2)), 0.05, 1.0)
    w_gate = noise(seeds[4], (EXPERTS, D, FF), D ** -0.5, 0.125, ((0, 8), (2, 2)))
    w_up = noise(seeds[5], (EXPERTS, D, FF), D ** -0.5, 0.125, ((0, 8), (2, 2)))
    w_down = noise(seeds[6], (EXPERTS, FF, D), FF ** -0.5, 0.078125, ((0, 8), (1, 2)))
    return {"tokens": tokens, "gain": gain, "routes": routes, "weights": weights, "w_gate": w_gate, "w_up": w_up, "w_down": w_down}


epsilon = 1e-05

def normalize(values, gain):
    values = values.astype(jnp.float32)
    average = lax.optimization_barrier(jnp.mean(values, axis=1, keepdims=True))
    spread = lax.optimization_barrier(jnp.mean(jnp.square(values - average), axis=1, keepdims=True))
    return ((values - average) * lax.rsqrt(spread + epsilon) * gain).astype(jnp.bfloat16)

def reference(tokens, gain, routes, weights, w_gate, w_up, w_down):
    normed = normalize(tokens, gain)
    pair_count = TOKENS * TOP
    pair_expert = routes.reshape(-1).astype(jnp.int32)
    member = (pair_expert[:, None] == jnp.arange(EXPERTS, dtype=jnp.int32)[None, :]).astype(jnp.int32)
    earlier = jnp.cumsum(member, axis=0) - member
    room = N_EP * CAP
    position = (pair_expert * room + lax.optimization_barrier(jnp.sum(earlier * member, axis=1))).astype(jnp.int32)
    owner = jnp.full((EXPERTS * room,), TOKENS, jnp.int32)
    owner = owner.at[position].set(jnp.arange(pair_count, dtype=jnp.int32) // TOP)
    padded = jnp.concatenate([normed, jnp.zeros((1, D), jnp.bfloat16)], axis=0)
    block_width = FF // N_TP

    def expert(operands):
        index, gate_w, up_w, down_w = operands
        chosen = padded[index]
        gate_val = jnp.dot(chosen, gate_w, preferred_element_type=jnp.float32)
        up_val = jnp.dot(chosen, up_w, preferred_element_type=jnp.float32)
        hidden = (jax.nn.silu(gate_val) * up_val).astype(jnp.bfloat16)
        hidden_blocks = hidden.reshape(room, N_TP, block_width)
        down_blocks = down_w.reshape(N_TP, block_width, D)

        def one_block(carry, block):
            part = jnp.dot(block[0], block[1], preferred_element_type=jnp.float32).astype(jnp.bfloat16)
            return (carry + part.astype(jnp.float32), None)
        total, unused = lax.scan(one_block, jnp.zeros((room, D), jnp.float32), (jnp.swapaxes(hidden_blocks, 0, 1), down_blocks))
        return total.astype(jnp.bfloat16)
    results = lax.map(expert, (owner.reshape(EXPERTS, room), w_gate, w_up, w_down))
    results = results.reshape(EXPERTS * room, D)
    picked = results[position].reshape(TOKENS, TOP, D).astype(jnp.float32)
    return lax.optimization_barrier(jnp.sum(picked * weights[:, :, None], axis=1)).astype(jnp.bfloat16)
```

```python
import functools

import jax
import jax.numpy as jnp
from jax import lax
from jax.experimental import pallas as pl
from jax.experimental.pallas import tpu as pltpu
from jax.sharding import PartitionSpec as P

epsilon = 1e-05
MESH = pl.DeviceIdType.MESH
BF = jnp.bfloat16
F32 = jnp.float32


def piece(total, most):
    best = 128
    for cand in range(128, min(total, most) + 1, 128):
        if total % cand == 0:
            best = cand
    return best


def kernel(dims, tok, gain, routes, weights, wg_hbm, wu_hbm, wd_hbm, out,
           xg, normed, hidden, wcol, wsrc, wrow, wg, wu, wd,
           psend, precv, sacc, xsend, xrecv, zsend, zrecv,
           wg_sem, wu_sem, wd_sem, gs, gr, ws, wr, ps, pr, xs, xr, zs, zr):
    n_ep, n_tp, X, Z, rows, w, FC, NF, CW, J, top = dims
    e = lax.axis_index("ep")
    t = lax.axis_index("tp")
    x = lax.rem(e, X)
    z = e // X
    xp = X - 1 - x

    def w_copy(kind, c):
        if kind == 2:
            return pltpu.make_async_copy(wd_hbm.at[0, :, pl.ds(c * CW, CW)], wd.at[c], wd_sem.at[c])
        src, dst, sem = ((wg_hbm, wg, wg_sem), (wu_hbm, wu, wu_sem))[kind]
        return pltpu.make_async_copy(src.at[0, :, pl.ds(c * FC, FC)], dst.at[c], sem.at[c])

    for c in range(NF):
        w_copy(0, c).start()
        w_copy(1, c).start()
    for c in range(n_tp * J):
        w_copy(2, c).start()

    def dev(ep, tp):
        return {"ep": ep, "tp": tp}

    barrier = pltpu.get_barrier_semaphore()
    for d in range(1, n_ep):
        pl.semaphore_signal(barrier, inc=1, device_id=dev(lax.rem(e + d, n_ep), t), device_id_type=MESH)
    for d in range(1, n_tp):
        pl.semaphore_signal(barrier, inc=1, device_id=dev(e, lax.rem(t + d, n_tp)), device_id_type=MESH)

    sub = lax.broadcasted_iota(jnp.int32, (rows, 128), 0)
    lane = lax.broadcasted_iota(jnp.int32, (rows, 128), 1)
    r = routes[...]
    wv = weights[...]
    for i in range(n_ep):
        col = jnp.sum(jnp.where(r == i, wv, 0.0), axis=1, keepdims=True)
        wsrc[i] = jnp.sum(jnp.where(sub == lane, col, 0.0), axis=0, keepdims=True)
    xg[e, t] = tok[...]
    wrow[e] = wsrc[e]

    pl.semaphore_wait(barrier, n_ep - 1 + n_tp - 1)

    def g_copy(kind, src, slot_e, target):
        return pltpu.make_async_remote_copy(
            src_ref=src, dst_ref=xg.at[slot_e, t], send_sem=gs.at[kind, slot_e],
            recv_sem=gr.at[slot_e, t], device_id=target, device_id_type=MESH)

    def targets(origin):
        res = []
        if origin in ("own", "low"):
            res.append((z < Z - 1, 0, dev(lax.rem(z + 1, Z) * X + x, t)))
        if origin in ("own", "high"):
            res.append((z > 0, 1, dev(lax.rem(z + Z - 1, Z) * X + x, t)))
        if origin != "across" and X > 1:
            res.append((None, 2, dev(z * X + xp, t)))
        for d in range(1, n_tp):
            res.append((None, 2 + d, dev(e, lax.rem(t + d, n_tp))))
        return res

    def forward(origin, slot_e, act):
        src = tok if origin == "own" else xg.at[slot_e, t]
        for cond, kind, target in targets(origin):
            cp = g_copy(kind, src, slot_e, target)
            fn = cp.start if act == "start" else cp.wait_send
            if cond is None:
                fn()
            else:
                pl.when(cond)(fn)

    def wait_slot(slot_e, slot_t):
        pltpu.make_async_remote_copy(
            src_ref=xg.at[slot_e, slot_t], dst_ref=xg.at[slot_e, slot_t], send_sem=gs.at[0, slot_e],
            recv_sem=gr.at[slot_e, slot_t], device_id=dev(e, t), device_id_type=MESH).wait_recv()

    def walk(act):
        forward("own", e, act)
        if act == "start":
            for d in range(1, n_ep):
                to = lax.rem(e + d, n_ep)
                pltpu.make_async_remote_copy(
                    src_ref=wsrc.at[to], dst_ref=wrow.at[e], send_sem=ws.at[to], recv_sem=wr.at[e],
                    device_id=dev(to, t), device_id_type=MESH).start()

        def handle(origin, slot_e):
            if act == "start":
                wait_slot(slot_e, t)
            forward(origin, slot_e, act)

        if X > 1:
            handle("across", z * X + xp)
        for d in range(1, Z):
            for origin, zz, cond in (("low", z - d, z >= d), ("high", z + d, z + d < Z)):
                pl.when(cond)(functools.partial(handle, origin, zz * X + x))
            if X > 1:
                for zz, cond in ((z - d, z >= d), (z + d, z + d < Z)):
                    pl.when(cond)(functools.partial(handle, "across", zz * X + xp))

    walk("start")

    def norm_step(i, carry):
        s = lax.rem(e + i, n_ep)

        @pl.when(i > 0)
        def _():
            pltpu.make_async_remote_copy(
                src_ref=wsrc.at[s], dst_ref=wrow.at[s], send_sem=ws.at[s], recv_sem=wr.at[s],
                device_id=dev(s, t), device_id_type=MESH).wait_recv()

        for d in range(1, n_tp):
            wait_slot(s, lax.rem(t + d, n_tp))
        parts = [xg[s, k].astype(F32) for k in range(n_tp)]
        width = w * n_tp
        mean = sum(jnp.sum(p, axis=1, keepdims=True) for p in parts) / width
        parts = [p - mean for p in parts]
        var = sum(jnp.sum(p * p, axis=1, keepdims=True) for p in parts) / width
        inv = lax.rsqrt(var + epsilon)
        at = pl.ds(pl.multiple_of(s * rows, rows), rows)
        for k in range(n_tp):
            normed[at, k * w:(k + 1) * w] = (parts[k] * inv * gain[:, k * w:(k + 1) * w]).astype(BF)
        wcol[at, :] = jnp.sum(jnp.where(sub == lane, wrow[s], 0.0), axis=1, keepdims=True)
        return carry

    lax.fori_loop(0, n_ep, norm_step, 0)

    def up_step(c, carry):
        w_copy(0, c).wait()
        gate_val = jnp.dot(normed[...], wg[c], preferred_element_type=F32)
        w_copy(1, c).wait()
        up_val = jnp.dot(normed[...], wu[c], preferred_element_type=F32)
        h = gate_val / (1.0 + jnp.exp(-gate_val)) * up_val * wcol[...]
        hidden[:, pl.ds(pl.multiple_of(c * FC, FC), FC)] = h.astype(BF)
        return carry

    lax.fori_loop(0, NF, up_step, 0)

    def p_copy(d, j):
        return pltpu.make_async_remote_copy(
            src_ref=psend.at[d - 1, j], dst_ref=precv.at[d - 1, j], send_sem=ps.at[d - 1, j],
            recv_sem=pr.at[d - 1, j], device_id=dev(e, lax.rem(t + d, n_tp)), device_id_type=MESH)

    def x_copy(j, zz):
        return pltpu.make_async_remote_copy(
            src_ref=xsend.at[j, zz], dst_ref=xrecv.at[j, zz], send_sem=xs.at[j, zz],
            recv_sem=xr.at[j, zz], device_id=dev(z * X + xp, t), device_id_type=MESH)

    def z_copy(j, d):
        return pltpu.make_async_remote_copy(
            src_ref=zsend.at[j, d - 1], dst_ref=zrecv.at[j, d - 1], send_sem=zs.at[j, d - 1],
            recv_sem=zr.at[j, d - 1], device_id=dev(lax.rem(z + d, Z) * X + x, t), device_id_type=MESH)

    def block(zz, xx):
        return pl.ds(pl.multiple_of((zz * X + xx) * rows, rows), rows)

    order = list(range(1, Z)) + [0]
    for d in list(range(1, n_tp)) + [0]:
        to = lax.rem(t + d, n_tp)
        for j in range(J):
            c = to * J + j
            w_copy(2, c).wait()
            acc = jnp.dot(hidden[...], wd[c], preferred_element_type=F32)
            if d:
                psend[d - 1, j] = acc.astype(BF)
                p_copy(d, j).start()
            else:
                for k in range(1, n_tp):
                    p_copy(k, j).wait_recv()
                    acc = acc + precv[k - 1, j].astype(F32)
                sacc[j] = acc
                if X > 1:
                    for dz in order:
                        zz = lax.rem(z + dz, Z)
                        xsend[j, zz] = sacc[j, block(zz, xp), :].astype(BF)
                        x_copy(j, zz).start()

    def summed(j, zz):
        total = sacc[j, block(zz, x), :]
        if X > 1:
            x_copy(j, zz).wait_recv()
            total = total + xrecv[j, zz].astype(F32)
        return total

    for j in range(J):
        for dz in range(1, Z):
            zsend[j, dz - 1] = summed(j, lax.rem(z + dz, Z)).astype(BF)
            z_copy(j, dz).start()
    for j in range(J):
        total = summed(j, z)
        for dz in range(1, Z):
            z_copy(j, dz).wait_recv()
            total = total + zrecv[j, dz - 1].astype(F32)
        out[:, j * CW:(j + 1) * CW] = total.astype(BF)

    walk("end")
    for d in range(1, n_ep):
        to = lax.rem(e + d, n_ep)
        pltpu.make_async_remote_copy(
            src_ref=wsrc.at[to], dst_ref=wrow.at[e], send_sem=ws.at[to], recv_sem=wr.at[e],
            device_id=dev(to, t), device_id_type=MESH).wait_send()
    for j in range(J):
        for d in range(1, n_tp):
            p_copy(d, j).wait_send()
        if X > 1:
            for zz in range(Z):
                x_copy(j, zz).wait_send()
        for dz in range(1, Z):
            z_copy(j, dz).wait_send()


def solution(mesh):
    n_ep, n_tp = mesh.shape["ep"], mesh.shape["tp"]
    X = 2 if n_ep % 2 == 0 else 1
    Z = n_ep // X

    def on_device(tokens, gain, routes, weights, w_gate, w_up, w_down):
        rows, w = tokens.shape
        D = w * n_tp
        top = routes.shape[1]
        F = w_gate.shape[2]
        FC = piece(F, 512)
        NF = F // FC
        CW = piece(w, 512)
        J = w // CW
        T = n_ep * rows
        dims = (n_ep, n_tp, X, Z, rows, w, FC, NF, CW, J, top)
        vm = pl.BlockSpec(memory_space=pltpu.VMEM)
        hbm = pl.BlockSpec(memory_space=pl.ANY)
        sem = pltpu.SemaphoreType.DMA
        tn, zn = max(n_tp - 1, 1), max(Z - 1, 1)
        return pl.pallas_call(
            functools.partial(kernel, dims),
            out_shape=jax.ShapeDtypeStruct((rows, w), BF),
            in_specs=[vm] * 4 + [hbm] * 3,
            out_specs=vm,
            scratch_shapes=[
                pltpu.VMEM((n_ep, n_tp, rows, w), BF),
                pltpu.VMEM((T, D), BF),
                pltpu.VMEM((T, F), BF),
                pltpu.VMEM((T, 1), F32),
                pltpu.VMEM((n_ep, 1, 128), F32),
                pltpu.VMEM((n_ep, 1, 128), F32),
                pltpu.VMEM((NF, D, FC), BF),
                pltpu.VMEM((NF, D, FC), BF),
                pltpu.VMEM((n_tp * J, F, CW), BF),
                pltpu.VMEM((tn, J, T, CW), BF),
                pltpu.VMEM((tn, J, T, CW), BF),
                pltpu.VMEM((J, T, CW), F32),
                pltpu.VMEM((J, Z, rows, CW), BF),
                pltpu.VMEM((J, Z, rows, CW), BF),
                pltpu.VMEM((J, zn, rows, CW), BF),
                pltpu.VMEM((J, zn, rows, CW), BF),
                sem((NF,)), sem((NF,)), sem((n_tp * J,)),
                sem((2 + n_tp, n_ep)), sem((n_ep, n_tp)),
                sem((n_ep,)), sem((n_ep,)),
                sem((tn, J)), sem((tn, J)),
                sem((J, Z)), sem((J, Z)),
                sem((J, zn)), sem((J, zn)),
            ],
            compiler_params=pltpu.CompilerParams(
                collective_id=0, has_side_effects=True, vmem_limit_bytes=62 << 20
            ),
        )(tokens, gain.reshape(1, -1), routes, weights, w_gate, w_up, w_down)

    in_specs = (
        P(("grp", "ep"), "tp"),
        P(),
        P(("grp", "ep"), None),
        P(("grp", "ep"), None),
        P("ep", None, "tp"),
        P("ep", None, "tp"),
        P("ep", "tp", None),
    )
    out_specs = P(("grp", "ep"), "tp")
    return jax.shard_map(
        on_device, mesh=mesh, in_specs=in_specs, out_specs=out_specs, check_vma=False
    )
```

```python
import functools

import jax
import jax.numpy as jnp
from jax import lax
from jax.experimental import pallas as pl
from jax.experimental.pallas import tpu as pltpu
from jax.sharding import PartitionSpec as P

epsilon = 1e-05
MESH = pl.DeviceIdType.MESH
BF = jnp.bfloat16
F32 = jnp.float32


def piece(total, most):
    best = 128
    for cand in range(128, min(total, most) + 1, 128):
        if total % cand == 0:
            best = cand
    return best


def kernel(dims, tok, gain, routes, weights, wg_hbm, wu_hbm, wd_hbm, out,
           xg, normed, hidden, wcol, wsrc, wrow, wg, wu, wd,
           psend, precv, sacc, xsend, xrecv, zsend, zrecv,
           wg_sem, wu_sem, wd_sem, gs, gr, ws, wr, ps, pr, xs, xr, zs, zr):
    n_ep, n_tp, X, Z, NB, rb, rows, w, FC, NF, CW, J = dims
    e = lax.axis_index("ep")
    t = lax.axis_index("tp")
    x = lax.rem(e, X)
    z = e // X
    xp = X - 1 - x

    def w_copy(kind, c):
        if kind == 2:
            return pltpu.make_async_copy(wd_hbm.at[0, :, pl.ds(c * CW, CW)], wd.at[c], wd_sem.at[c])
        src, dst, sem = ((wg_hbm, wg, wg_sem), (wu_hbm, wu, wu_sem))[kind]
        return pltpu.make_async_copy(src.at[0, :, pl.ds(c * FC, FC)], dst.at[c], sem.at[c])

    for c in range(NF):
        w_copy(0, c).start()
        w_copy(1, c).start()
    for c in range(n_tp * J):
        w_copy(2, c).start()

    def dev(ep, tp):
        return {"ep": ep, "tp": tp}

    barrier = pltpu.get_barrier_semaphore()
    for d in range(1, n_ep):
        pl.semaphore_signal(barrier, inc=1, device_id=dev(lax.rem(e + d, n_ep), t), device_id_type=MESH)
    for d in range(1, n_tp):
        pl.semaphore_signal(barrier, inc=1, device_id=dev(e, lax.rem(t + d, n_tp)), device_id_type=MESH)

    r = routes[...]
    wv = weights[...]
    for i in range(n_ep):
        wsrc[i] = jnp.sum(jnp.where(r == i, wv, 0.0), axis=0, keepdims=True)
    for b in range(NB):
        xg[b, e, t] = tok[b * rb:(b + 1) * rb]
    wrow[e] = wsrc[e]

    pl.semaphore_wait(barrier, n_ep - 1 + n_tp - 1)

    def g_copy(b, kind, src, slot_e, target):
        return pltpu.make_async_remote_copy(
            src_ref=src, dst_ref=xg.at[b, slot_e, t], send_sem=gs.at[b, kind, slot_e],
            recv_sem=gr.at[b, slot_e, t], device_id=target, device_id_type=MESH)

    def sends(b, origin, slot_e):
        src = tok.at[pl.ds(b * rb, rb)] if origin == "own" else xg.at[b, slot_e, t]
        res = []
        if origin == "own":
            for d in far:
                res.append(g_copy(b, d - 1, src, slot_e, dev(lax.rem(z + d, Z) * X + x, t)))
        if origin != "across" and X > 1:
            res.append(g_copy(b, Z - 1, src, slot_e, dev(z * X + xp, t)))
        for d in range(1, n_tp):
            res.append(g_copy(b, Z - 1 + d, src, slot_e, dev(e, lax.rem(t + d, n_tp))))
        return res

    def route_copy(to):
        return pltpu.make_async_remote_copy(
            src_ref=wsrc.at[to], dst_ref=wrow.at[e], send_sem=ws.at[to], recv_sem=wr.at[e],
            device_id=dev(to, t), device_id_type=MESH)

    def wait_slot(b, slot_e, slot_t):
        pltpu.make_async_remote_copy(
            src_ref=xg.at[b, slot_e, slot_t], dst_ref=xg.at[b, slot_e, slot_t], send_sem=gs.at[b, 0, slot_e],
            recv_sem=gr.at[b, slot_e, slot_t], device_id=dev(e, t), device_id_type=MESH).wait_recv()

    far = list(range(1, Z))

    def relay(b, origin, slot_e):
        wait_slot(b, slot_e, t)
        for cp in sends(b, origin, slot_e):
            cp.start()

    def relay_near(b):
        for d in far:
            relay(b, "along", lax.rem(z + d, Z) * X + x)

    def relay_across(b):
        if X > 1:
            for d in [0] + far:
                relay(b, "across", lax.rem(z + d, Z) * X + xp)

    def norm(b):
        diag = (lax.broadcasted_iota(jnp.int32, (rb, rows), 0) + b * rb
                == lax.broadcasted_iota(jnp.int32, (rb, rows), 1))

        def arrive(i, carry):
            s = lax.rem(e + i, n_ep)
            if b == 0:
                @pl.when(i > 0)
                def _():
                    pltpu.make_async_remote_copy(
                        src_ref=wsrc.at[s], dst_ref=wrow.at[s], send_sem=ws.at[s], recv_sem=wr.at[s],
                        device_id=dev(s, t), device_id_type=MESH).wait_recv()

            for d in range(1, n_tp):
                wait_slot(b, s, lax.rem(t + d, n_tp))
            return carry

        def norm_step(s, carry):
            parts = [xg[b, s, k].astype(F32) for k in range(n_tp)]
            width = w * n_tp
            mean = sum(jnp.sum(p, axis=1, keepdims=True) for p in parts) / width
            parts = [p - mean for p in parts]
            var = sum(jnp.sum(p * p, axis=1, keepdims=True) for p in parts) / width
            inv = lax.rsqrt(var + epsilon)
            at = pl.ds(pl.multiple_of(s * rb, rb), rb)
            for k in range(n_tp):
                normed[b, at, k * w:(k + 1) * w] = (
                    parts[k] * inv * gain[:, k * w:(k + 1) * w]).astype(BF)
            wcol[b, at, :] = jnp.sum(jnp.where(diag, wrow[s], 0.0), axis=1, keepdims=True)
            return carry

        lax.fori_loop(0, n_ep, arrive, 0)
        lax.fori_loop(0, n_ep, norm_step, 0, unroll=4)

    def up(b, between):
        def up_step(c, carry):
            if b == 0:
                w_copy(0, c).wait()
            gate_val = jnp.dot(normed[b], wg[c], preferred_element_type=F32)
            if b == 0:
                w_copy(1, c).wait()
            up_val = jnp.dot(normed[b], wu[c], preferred_element_type=F32)
            h = gate_val / (1.0 + jnp.exp(-gate_val)) * up_val * wcol[b]
            hidden[b, :, pl.ds(pl.multiple_of(c * FC, FC), FC)] = h.astype(BF)
            for at, fn in between:
                pl.when(c == min(at, NF - 1))(fn)
            return carry

        lax.fori_loop(0, NF, up_step, 0)

    def p_copy(b, d, j):
        return pltpu.make_async_remote_copy(
            src_ref=psend.at[b, d - 1, j], dst_ref=precv.at[b, d - 1, j], send_sem=ps.at[b, d - 1, j],
            recv_sem=pr.at[b, d - 1, j], device_id=dev(e, lax.rem(t + d, n_tp)), device_id_type=MESH)

    def x_copy(b, j, zz):
        return pltpu.make_async_remote_copy(
            src_ref=xsend.at[b, j, zz], dst_ref=xrecv.at[b, j, zz], send_sem=xs.at[b, j, zz],
            recv_sem=xr.at[b, j, zz], device_id=dev(z * X + xp, t), device_id_type=MESH)

    def z_copy(b, j, d):
        return pltpu.make_async_remote_copy(
            src_ref=zsend.at[b, j, d - 1], dst_ref=zrecv.at[b, j, d - 1], send_sem=zs.at[b, j, d - 1],
            recv_sem=zr.at[b, j, d - 1], device_id=dev(lax.rem(z + d, Z) * X + x, t), device_id_type=MESH)

    def block(zz, xx):
        return pl.ds(pl.multiple_of((zz * X + xx) * rb, rb), rb)

    def down(b):
        for j in range(J):
            for d in list(range(1, n_tp)) + [0]:
                to = lax.rem(t + d, n_tp)
                c = to * J + j
                if b == 0:
                    w_copy(2, c).wait()
                acc = jnp.dot(hidden[b], wd[c], preferred_element_type=F32)
                if d:
                    psend[b, d - 1, j] = acc.astype(BF)
                    p_copy(b, d, j).start()
                else:
                    for k in range(1, n_tp):
                        p_copy(b, k, j).wait_recv()
                        acc = acc + precv[b, k - 1, j].astype(F32)
                    sacc[b, j] = acc
                    if X > 1:
                        for dz in far + [0]:
                            zz = lax.rem(z + dz, Z)
                            xsend[b, j, zz] = sacc[b, j, block(zz, xp), :].astype(BF)
                            x_copy(b, j, zz).start()

    def summed(b, j, zz):
        total = sacc[b, j, block(zz, x), :]
        if X > 1:
            x_copy(b, j, zz).wait_recv()
            total = total + xrecv[b, j, zz].astype(F32)
        return total

    def along(b):
        for j in range(J):
            for dz in far:
                zsend[b, j, dz - 1] = summed(b, j, lax.rem(z + dz, Z)).astype(BF)
                z_copy(b, j, dz).start()

    def finish(b):
        for j in range(J):
            total = summed(b, j, z)
            for dz in far:
                z_copy(b, j, dz).wait_recv()
                total = total + zrecv[b, j, dz - 1].astype(F32)
            out[b * rb:(b + 1) * rb, j * CW:(j + 1) * CW] = total.astype(BF)

    def begin(b):
        for cp in sends(b, "own", e):
            cp.start()

    begin(0)
    for d in range(1, n_ep):
        route_copy(lax.rem(e + d, n_ep)).start()
    relay_near(0)
    for b in range(1, NB):
        begin(b)
    relay_across(0)
    norm(0)
    for b in range(NB):
        between = []
        if b > 0:
            between.append((NF - 1, functools.partial(along, b - 1)))
        if b + 1 < NB:
            between.append((NF // 2, functools.partial(relay_near, b + 1)))
            between.append((NF - 1, functools.partial(relay_across, b + 1)))
        up(b, between)
        if b + 1 < NB:
            norm(b + 1)
        down(b)
    along(NB - 1)
    for b in range(NB):
        finish(b)

    for b in range(NB):
        for cp in sends(b, "own", e):
            cp.wait_send()
        for d in far:
            for cp in sends(b, "along", lax.rem(z + d, Z) * X + x):
                cp.wait_send()
        if X > 1:
            for d in range(Z):
                for cp in sends(b, "across", lax.rem(z + d, Z) * X + xp):
                    cp.wait_send()
        for j in range(J):
            for d in range(1, n_tp):
                p_copy(b, d, j).wait_send()
            if X > 1:
                for zz in range(Z):
                    x_copy(b, j, zz).wait_send()
            for dz in far:
                z_copy(b, j, dz).wait_send()
    for d in range(1, n_ep):
        route_copy(lax.rem(e + d, n_ep)).wait_send()


def solution(mesh):
    n_ep, n_tp = mesh.shape["ep"], mesh.shape["tp"]
    X = 2 if n_ep % 2 == 0 else 1
    Z = n_ep // X

    def on_device(tokens, gain, routes, weights, w_gate, w_up, w_down):
        rows, w = tokens.shape
        D = w * n_tp
        F = w_gate.shape[2]
        FC = piece(F, 512)
        NF = F // FC
        CW = piece(w, 512)
        J = w // CW
        NB = 1
        rb = rows // NB
        T = n_ep * rb
        dims = (n_ep, n_tp, X, Z, NB, rb, rows, w, FC, NF, CW, J)
        vm = pl.BlockSpec(memory_space=pltpu.VMEM)
        hbm = pl.BlockSpec(memory_space=pl.ANY)
        sem = pltpu.SemaphoreType.DMA
        tn, zn = max(n_tp - 1, 1), max(Z - 1, 1)
        return pl.pallas_call(
            functools.partial(kernel, dims),
            out_shape=jax.ShapeDtypeStruct((rows, w), BF),
            in_specs=[vm] * 4 + [hbm] * 3,
            out_specs=vm,
            scratch_shapes=[
                pltpu.VMEM((NB, n_ep, n_tp, rb, w), BF),
                pltpu.VMEM((NB, T, D), BF),
                pltpu.VMEM((NB, T, F), BF),
                pltpu.VMEM((NB, T, 1), F32),
                pltpu.VMEM((n_ep, 1, rows), F32),
                pltpu.VMEM((n_ep, 1, rows), F32),
                pltpu.VMEM((NF, D, FC), BF),
                pltpu.VMEM((NF, D, FC), BF),
                pltpu.VMEM((n_tp * J, F, CW), BF),
                pltpu.VMEM((NB, tn, J, T, CW), BF),
                pltpu.VMEM((NB, tn, J, T, CW), BF),
                pltpu.VMEM((NB, J, T, CW), F32),
                pltpu.VMEM((NB, J, Z, rb, CW), BF),
                pltpu.VMEM((NB, J, Z, rb, CW), BF),
                pltpu.VMEM((NB, J, zn, rb, CW), BF),
                pltpu.VMEM((NB, J, zn, rb, CW), BF),
                sem((NF,)), sem((NF,)), sem((n_tp * J,)),
                sem((NB, Z + n_tp - 1, n_ep)), sem((NB, n_ep, n_tp)),
                sem((n_ep,)), sem((n_ep,)),
                sem((NB, tn, J)), sem((NB, tn, J)),
                sem((NB, J, Z)), sem((NB, J, Z)),
                sem((NB, J, zn)), sem((NB, J, zn)),
            ],
            compiler_params=pltpu.CompilerParams(
                collective_id=0, has_side_effects=True, vmem_limit_bytes=62 << 20
            ),
        )(tokens, gain.reshape(1, -1), routes.T, weights.T, w_gate, w_up, w_down)

    in_specs = (
        P(("grp", "ep"), "tp"),
        P(),
        P(("grp", "ep"), None),
        P(("grp", "ep"), None),
        P("ep", None, "tp"),
        P("ep", None, "tp"),
        P("ep", "tp", None),
    )
    out_specs = P(("grp", "ep"), "tp")
    return jax.shard_map(
        on_device, mesh=mesh, in_specs=in_specs, out_specs=out_specs, check_vma=False
    )
```
